32 devices in a mesh: sp: 8 (over z, y), tp: 4 (over x, core).
Axes of the slice: x: 2, y: 2, z: 4, core: 2. Of those that a mesh axis runs over, the one named last changes fastest.
Arguments:
- latents: bfloat16 [2560, 2048], P(('sp', 'tp')), may hold values from -12.5 to 12.5, as said below
- context: bfloat16 [1024, 2048], P('sp'), may hold values from -120 to 120, as said below
- cond_vec: float32 [2048], replicated, may hold values from -6 to 6
- ctx_vec: float32 [2048], replicated, may hold values from -6 to 6
- shift_w: bfloat16 [2048, 2048], P('sp', 'tp'), may hold values from -0.125 to 0.125
- scale_w: bfloat16 [2048, 2048], P('sp', 'tp'), may hold values from -0.125 to 0.125
- modgate_w: bfloat16 [2048, 2048], P('sp', 'tp'), may hold values from -0.125 to 0.125
- query_down_weight: bfloat16 [2048, 512], replicated, may hold values from -0.125 to 0.125
- latent_down_weight: bfloat16 [2048, 256], replicated, may hold values from -0.125 to 0.125
- rot_down: bfloat16 [2048, 32], replicated, may hold values from -0.125 to 0.125
- gate_w: bfloat16 [2048, 2048], P(None, 'tp'), may hold values from -0.125 to 0.125
- query_norm_gain: float32 [512], replicated, may hold values from 0.1 to 1.9
- latent_norm_gain: float32 [256], replicated, may hold values from 0.1 to 1.9
- query_plain_weight: bfloat16 [512, 2048], P(None, 'tp'), may hold values from -0.25 to 0.25
- query_rotary_weight: bfloat16 [512, 1024], P(None, 'tp'), may hold values from -0.25 to 0.25
- key_expand_weight: bfloat16 [256, 2048], P(None, 'tp'), may hold values from -0.375 to 0.375
- value_expand_weight: bfloat16 [256, 2048], P(None, 'tp'), may hold values from -0.375 to 0.375
- out_w: bfloat16 [2048, 2048], P('tp'), may hold values from -0.5 to 0.5
- norm_gain: float32 [2048], replicated, may hold values from 0.1 to 1.9
- norm_bias: float32 [2048], replicated, may hold values from -3 to 3
Outputs:
- mixed_out: bfloat16 [2560, 2048], P(('sp', 'tp'))
The draws below stay inside these ranges and needn't reach their ends.
Inputs may be any that keep to these rules, and one draw needn't show every extreme that they name: `latents`: latent rows are noise plus three slow waves along the whole sequence. Most context rows have their own scales of 1 to 3; a few rows may be far larger.
All inputs are finite; a program needn't handle non-finite values.
Results may differ from the reference program's by a relative error of at most 0.024.
The reference program's roundings to bfloat16 on the way count: a program that leaves them out, or rounds other values in their place, can miss the bound.
Values may be sent and summed in bfloat16 or wider, within the bound.
No kernel may reach another device: no remote copies, remote signals or barrier semaphores. Data moves between devices by JAX's collectives and lax.ppermute only.
A program may use at most 128 MiB of HBM per device.

```python
import math
import jax
import jax.numpy as jnp
from jax import lax

MODEL_WIDTH = 2048
HEAD_COUNT = 32
QUERY_LATENT = 512
LATENT_WIDTH = 256
PLAIN_HEAD_SIZE = 64
ROTARY_SIZE = 32
VALUE_HEAD_SIZE = 64
GRID_W = 64
TOK_DEV = 320
CTX = 1024
TOKENS = 2560
N_TP = 4


def draw_latents(key, part):
    noise_key, wave_key, phase_key = jax.random.split(key, 3)
    noise_part = jnp.clip(jax.random.normal(noise_key, (TOKENS, MODEL_WIDTH), jnp.float32), -5.0, 5.0)
    directions = jnp.clip(jax.random.normal(wave_key, (3, MODEL_WIDTH), jnp.float32), -2.5, 2.5)
    phases = jax.random.uniform(phase_key, (3,), jnp.float32, 0.0, 2.0 * math.pi)
    position = jnp.arange(TOKENS, dtype=jnp.float32) / TOKENS
    frequency = jnp.arange(1, 4, dtype=jnp.float32)
    wave_part = jnp.cos(2.0 * math.pi * position[:, None] * frequency[None, :] + phases[None, :])
    return (noise_part + wave_part @ directions).astype(jnp.bfloat16)


def draw_context(key, part):
    value_key, scale_key, pick_key, large_key = jax.random.split(key, 4)
    row_scale = jnp.exp(jax.random.uniform(scale_key, (CTX, 1), jnp.float32, 0.0, math.log(3.0)))
    values = jnp.clip(jax.random.normal(value_key, (CTX, MODEL_WIDTH), jnp.float32), -6.0, 6.0) * row_scale
    return values.astype(jnp.bfloat16)


def level_of(own_key, shape, cuts, smallest, largest):
    loudness, own = 1.0, jax.random.fold_in(own_key, 6)
    for dim, blocks in cuts:
        heights = jnp.exp(jax.random.uniform(jax.random.fold_in(own, dim), (blocks,), jnp.float32, smallest / len(cuts), largest / len(cuts)))
        loudness = loudness * jnp.repeat(heights, shape[dim] // blocks).reshape([-1 if axis == dim else 1 for axis in range(len(shape))])
    return loudness


def bell_draw(rng, extent, scale, limit, cuts=(), kind=jnp.bfloat16):
    factor_of = level_of(rng, extent, cuts, -0.22, 0.18) if cuts else 1.0
    drawn = jax.random.normal(rng, extent, jnp.float32) * scale * factor_of
    return jnp.minimum(jnp.maximum(drawn, -limit), limit).astype(kind)


def setup_inputs(seed: int = 0) -> dict:
    keys = jax.random.split(jax.random.key(seed), 21)
    return {
        "latents": draw_latents(jax.random.fold_in(keys[20], 71), 0),
        "context": draw_context(jax.random.fold_in(keys[20], 71), 0),
        "cond_vec": bell_draw(keys[2], (MODEL_WIDTH,), 1.0, 6.0, (), jnp.float32),
        "ctx_vec": bell_draw(keys[3], (MODEL_WIDTH,), 1.0, 6.0, (), jnp.float32),
        "shift_w": bell_draw(keys[4], (MODEL_WIDTH, MODEL_WIDTH), MODEL_WIDTH ** -0.5, 0.125, ((0, 8), (1, 4))),
        "scale_w": bell_draw(keys[5], (MODEL_WIDTH, MODEL_WIDTH), MODEL_WIDTH ** -0.5, 0.125, ((0, 8), (1, 4))),
        "modgate_w": bell_draw(keys[6], (MODEL_WIDTH, MODEL_WIDTH), MODEL_WIDTH ** -0.5, 0.125, ((0, 8), (1, 4))),
        "query_down_weight": bell_draw(keys[7], (MODEL_WIDTH, QUERY_LATENT), MODEL_WIDTH ** -0.5, 0.125),
        "latent_down_weight": bell_draw(keys[8], (MODEL_WIDTH, LATENT_WIDTH), MODEL_WIDTH ** -0.5, 0.125),
        "rot_down": bell_draw(keys[9], (MODEL_WIDTH, ROTARY_SIZE), MODEL_WIDTH ** -0.5, 0.125),
        "gate_w": bell_draw(keys[10], (MODEL_WIDTH, HEAD_COUNT * VALUE_HEAD_SIZE), MODEL_WIDTH ** -0.5, 0.125, ((1, 4),)),
        "query_norm_gain": jnp.clip(1.0 + 0.18 * jax.random.normal(keys[11], (QUERY_LATENT,), jnp.float32), 0.1, 1.9),
        "latent_norm_gain": jnp.clip(1.0 + 0.18 * jax.random.normal(keys[12], (LATENT_WIDTH,), jnp.float32), 0.1, 1.9),
        "query_plain_weight": bell_draw(keys[13], (QUERY_LATENT, HEAD_COUNT * PLAIN_HEAD_SIZE), QUERY_LATENT ** -0.5, 0.25, ((1, 4),)),
        "query_rotary_weight": bell_draw(keys[14], (QUERY_LATENT, HEAD_COUNT * ROTARY_SIZE), QUERY_LATENT ** -0.5, 0.25, ((1, 4),)),
        "key_expand_weight": bell_draw(keys[15], (LATENT_WIDTH, HEAD_COUNT * PLAIN_HEAD_SIZE), LATENT_WIDTH ** -0.5, 0.375, ((1, 4),)),
        "value_expand_weight": bell_draw(keys[16], (LATENT_WIDTH, HEAD_COUNT * VALUE_HEAD_SIZE), LATENT_WIDTH ** -0.5, 0.375, ((1, 4),)),
        "out_w": bell_draw(keys[17], (HEAD_COUNT * VALUE_HEAD_SIZE, MODEL_WIDTH), (HEAD_COUNT * VALUE_HEAD_SIZE // 16) ** -0.5, 0.5, ((0, 4),)),
        "norm_gain": jnp.clip(1.0 + 0.18 * jax.random.normal(keys[18], (MODEL_WIDTH,), jnp.float32), 0.1, 1.9),
        "norm_bias": bell_draw(keys[19], (MODEL_WIDTH,), 0.5, 3.0, (), jnp.float32),
    }


rope_base = 10000.0
norm_floor = 1e-06
residual_weight = 2.0 ** 0.5

def rms_scale(values, gain):
    return values * lax.rsqrt(lax.optimization_barrier(jnp.mean(values * values, axis=-1, keepdims=True)) + norm_floor) * gain

def rotate(values, positions):
    pair_count = ROTARY_SIZE // 4
    inverse = rope_base ** (-jnp.arange(pair_count, dtype=jnp.float32) / pair_count)
    grid_row = (positions // GRID_W).astype(jnp.float32)
    grid_col = (positions % GRID_W).astype(jnp.float32)
    angles = jnp.stack([grid_row[:, None] * inverse, grid_col[:, None] * inverse], axis=1)
    cosine = jnp.cos(angles)[:, None, :, None, :]
    sine_part = jnp.sin(angles)[:, None, :, None, :]
    shaped = values.reshape(values.shape[0], -1, 2, 2, pair_count)
    first_part = shaped[:, :, :, 0:1, :]
    second = shaped[:, :, :, 1:2, :]
    turned = jnp.concatenate([first_part * cosine - second * sine_part, second * cosine + first_part * sine_part], axis=3)
    return turned.reshape(values.shape)

def project(rows, weight):
    return jnp.dot(rows, weight, preferred_element_type=jnp.float32)

def reference(latents, context, cond_vec, ctx_vec, shift_w, scale_w, modgate_w, query_down_weight, latent_down_weight, rot_down, gate_w, query_norm_gain, latent_norm_gain, query_plain_weight, query_rotary_weight, key_expand_weight, value_expand_weight, out_w, norm_gain, norm_bias):
    cond_rows = jnp.stack([jax.nn.silu(cond_vec), jax.nn.silu(ctx_vec)]).astype(jnp.bfloat16)
    shift_vec = project(cond_rows, shift_w)
    scale_vec = project(cond_rows, scale_w)
    gate_vec = project(cond_rows, modgate_w)
    latent_in = (latents.astype(jnp.float32) * (1.0 + scale_vec[0]) + shift_vec[0]).astype(jnp.bfloat16)
    context_in = (context.astype(jnp.float32) * (1.0 + scale_vec[1]) + shift_vec[1]).astype(jnp.bfloat16)
    positions = jnp.arange(TOKENS, dtype=jnp.int32)
    q_codes = rms_scale(project(latent_in, query_down_weight), query_norm_gain).astype(jnp.bfloat16)
    q_cont = project(q_codes, query_plain_weight).astype(jnp.bfloat16).reshape(TOKENS, HEAD_COUNT, PLAIN_HEAD_SIZE)
    q_rot = rotate(project(q_codes, query_rotary_weight), positions).astype(jnp.bfloat16).reshape(TOKENS, HEAD_COUNT, ROTARY_SIZE)
    gate_act = project(latent_in, gate_w).astype(jnp.bfloat16)
    all_in = jnp.concatenate([context_in, latent_in], axis=0)
    kv_codes = rms_scale(project(all_in, latent_down_weight), latent_norm_gain).astype(jnp.bfloat16)
    key_rot = jnp.concatenate([project(context_in, rot_down), rotate(project(latent_in, rot_down), positions)], axis=0).astype(jnp.bfloat16)
    key_rows = project(kv_codes, key_expand_weight).astype(jnp.bfloat16).reshape(-1, HEAD_COUNT, PLAIN_HEAD_SIZE).astype(jnp.float32)
    value_rows = project(kv_codes, value_expand_weight).astype(jnp.bfloat16).reshape(-1, HEAD_COUNT, VALUE_HEAD_SIZE).astype(jnp.float32)
    rot_wide = key_rot.astype(jnp.float32)
    score_scale = (PLAIN_HEAD_SIZE + ROTARY_SIZE) ** (-0.5)
    block_rows = TOK_DEV // N_TP

    def attend_block(inputs):
        cont_block, rot_block = inputs
        scores = jnp.einsum('qhd,khd->hqk', cont_block.astype(jnp.float32), key_rows)
        scores = (scores + jnp.einsum('qhd,kd->hqk', rot_block.astype(jnp.float32), rot_wide)) * score_scale
        weights = jnp.exp(scores - lax.optimization_barrier(jnp.max(scores, axis=-1, keepdims=True)))
        weights_low = lax.optimization_barrier(weights.astype(jnp.bfloat16)).astype(jnp.float32)
        weighted = jnp.einsum('hqk,khd->qhd', weights_low, value_rows)
        return weighted / jnp.transpose(lax.optimization_barrier(jnp.sum(weights, axis=-1)))[:, :, None]
    blocks = TOKENS // block_rows
    attended = lax.map(attend_block, (q_cont.reshape(blocks, block_rows, HEAD_COUNT, PLAIN_HEAD_SIZE), q_rot.reshape(blocks, block_rows, HEAD_COUNT, ROTARY_SIZE)))
    attended = attended.reshape(TOKENS, HEAD_COUNT * VALUE_HEAD_SIZE)
    gated = (attended * jax.nn.silu(gate_act.astype(jnp.float32))).astype(jnp.bfloat16)
    branch = project(gated, out_w)
    blended = residual_weight * latents.astype(jnp.float32) + gate_vec[0] * branch
    row_mean = lax.optimization_barrier(jnp.mean(blended, axis=-1, keepdims=True))
    centred = blended - row_mean
    row_var = lax.optimization_barrier(jnp.mean(centred * centred, axis=-1, keepdims=True))
    return (centred * lax.rsqrt(row_var + norm_floor) * norm_gain + norm_bias).astype(jnp.bfloat16)
```

```python
import math

import jax
import jax.numpy as jnp
from jax import lax
from jax.experimental import pallas as pl
from jax.experimental.pallas import tpu as pltpu
from jax.sharding import PartitionSpec as P

PLAIN = 64
ROT = 32
VALUE = 64
GRID_W = 64
LANES = 128
GROUP = 16
ROPE_BASE = 10000.0
FLOOR = 1e-06
RESIDUAL = 2.0**0.5
NEG = -1e30

VMEM = pl.BlockSpec(memory_space=pltpu.VMEM)
SMEM = pl.BlockSpec(memory_space=pltpu.SMEM)
PARAMS = pltpu.CompilerParams(vmem_limit_bytes=56 * 2**20)


def dot(a, b):
    return lax.dot_general(a, b, (((1,), (0,)), ((), ())), preferred_element_type=jnp.float32)


def dot_t(a, b):
    return lax.dot_general(a, b, (((1,), (1,)), ((), ())), preferred_element_type=jnp.float32)


def round_up(value, step):
    return -(-value // step) * step


def cost(flops, moved):
    return pl.CostEstimate(flops=flops, transcendentals=0, bytes_accessed=moved)


def lane_index(shape):
    return lax.broadcasted_iota(jnp.int32, shape, len(shape) - 1)


def turn(values, cosine, sine):
    width = values.shape[1]
    upper = pltpu.roll(values, width - 8, 1)
    lower = pltpu.roll(values, 8, 1)
    swapped = jnp.where((lane_index(values.shape) & 8) == 0, upper, lower)
    return values * cosine + swapped * sine


def rms(values, gain):
    return values * lax.rsqrt(jnp.mean(values * values, axis=-1, keepdims=True) + FLOOR) * gain


def mod_kernel(cond_ref, shift_ref, scale_ref, gate_ref, out_ref):
    rows = cond_ref[...]
    rows = (rows * (1.0 / (1.0 + jnp.exp(-rows)))).astype(jnp.bfloat16)
    out_ref[0:2, :] = dot(rows, shift_ref[...])[0:2, :]
    out_ref[2:4, :] = dot(rows, scale_ref[...])[0:2, :]
    out_ref[4:6, :] = dot(rows, gate_ref[...])[0:2, :]
    out_ref[6:8, :] = jnp.zeros((2, out_ref.shape[1]), jnp.float32)


def fill_mod(me_ref, pieces_ref, mod_ref, xors):
    width = pieces_ref.shape[-1]
    for place, xor in enumerate(xors):
        column = pl.multiple_of((me_ref[0] ^ xor) * width, LANES)
        mod_ref[:, pl.ds(column, width)] = pieces_ref[place]


def codes_kernel(xors, me_ref, mod_ref, lat_ref, ctx_ref, w_ref, gain_ref, cos_ref, sin_ref, out_ref, vec_ref, rows_ref):
    fill_mod(me_ref, mod_ref, vec_ref, xors)
    lat_rows, ctx_rows = lat_ref.shape[0], ctx_ref.shape[0]
    unit = rows_ref.shape[0]
    latent = gain_ref.shape[1]
    rows_ref[0:lat_rows, :] = lat_ref[...].astype(jnp.float32) * (1.0 + vec_ref[2:3, :]) + vec_ref[0:1, :]
    rows_ref[lat_rows : lat_rows + ctx_rows, :] = ctx_ref[...].astype(jnp.float32) * (1.0 + vec_ref[3:4, :]) + vec_ref[1:2, :]
    if lat_rows + ctx_rows < unit:
        rows_ref[lat_rows + ctx_rows :, :] = jnp.zeros((unit - lat_rows - ctx_rows, rows_ref.shape[1]), jnp.float32)
    both = dot(rows_ref[...].astype(jnp.bfloat16), w_ref[...])
    out_ref[0:unit, :] = rms(both[:, :latent], gain_ref[...]).astype(jnp.bfloat16)
    turned = turn(both[:, latent:], cos_ref[...], sin_ref[...])
    lanes = lane_index((GROUP, LANES))
    tiles = []
    for tile in range(latent // LANES):
        packed = jnp.zeros((GROUP, LANES), jnp.float32)
        for slot in range(LANES // ROT):
            group = tile * (LANES // ROT) + slot
            if group * GROUP < unit:
                piece = turned[group * GROUP : (group + 1) * GROUP, :]
                if slot:
                    piece = pltpu.roll(piece, slot * ROT, 1)
                packed = jnp.where((lanes // ROT) == slot, piece, packed)
        tiles.append(packed)
    out_ref[unit:, :] = jnp.concatenate(tiles, axis=1).astype(jnp.bfloat16)


def modulate_blocks(vec_ref, blocks, rows_ref):
    count = blocks[0].shape[0]
    for place, block in enumerate(blocks):
        rows_ref[place * count : (place + 1) * count, :] = block[...].astype(jnp.float32) * (1.0 + vec_ref[2:3, :]) + vec_ref[0:1, :]


def query_kernel(xors, *refs):
    n = len(xors)
    me_ref, mod_ref = refs[:2]
    blocks = refs[2 : 2 + n]
    down_ref, gain_ref, plain_ref, rotary_ref, cos_ref, sin_ref, out_ref, vec_ref, rows_ref = refs[2 + n :]
    fill_mod(me_ref, mod_ref, vec_ref, xors)
    modulate_blocks(vec_ref, blocks, rows_ref)
    codes = rms(dot(rows_ref[...].astype(jnp.bfloat16), down_ref[...]), gain_ref[...]).astype(jnp.bfloat16)
    content = dot(codes, plain_ref[...])
    rotary = dot(codes, rotary_ref[...])
    heads = out_ref.shape[0]
    lanes = lane_index((content.shape[0], LANES))
    per_tile = LANES // ROT
    for tile in range(heads // per_tile):
        turned = turn(rotary[:, tile * LANES : (tile + 1) * LANES], cos_ref[...], sin_ref[...])
        for slot in range(per_tile):
            head = tile * per_tile + slot
            pair = content[:, (head // 2) * LANES : (head // 2 + 1) * LANES]
            goal = PLAIN if head % 2 == 0 else 0
            shift = (goal - slot * ROT) % LANES
            moved = pltpu.roll(turned, shift, 1) if shift else turned
            if head % 2 == 0:
                joined = jnp.where(lanes < PLAIN, pair, jnp.where(lanes < PLAIN + ROT, moved, 0.0))
            else:
                joined = jnp.where(lanes >= PLAIN, pair, jnp.where(lanes < ROT, moved, 0.0))
            out_ref[head] = joined.astype(jnp.bfloat16)


def gate_kernel(xors, *refs):
    n = len(xors)
    me_ref, mod_ref = refs[:2]
    blocks = refs[2 : 2 + n]
    w_ref, out_ref, vec_ref, rows_ref = refs[2 + n :]
    fill_mod(me_ref, mod_ref, vec_ref, xors)
    modulate_blocks(vec_ref, blocks, rows_ref)
    out_ref[...] = dot(rows_ref[...].astype(jnp.bfloat16), w_ref[...]).astype(jnp.bfloat16)


def attend_kernel(n_kv, unit, valid, first, last, *refs):
    q_ref = refs[0]
    kv_refs = refs[1 : 1 + n_kv]
    at = 1 + n_kv
    key_w_ref, value_w_ref = refs[at : at + 2]
    at += 2
    if not first:
        state_ref = refs[at]
        at += 1
    if last:
        gate_ref = refs[at]
        at += 1
        keep_ref, send_ref = refs[at : at + 2]
        at += 2
    else:
        new_ref = refs[at]
        at += 1
    rot_ref, key_ref, val_ref = refs[at : at + 3]
    factor = (PLAIN + ROT) ** (-0.5) * math.log2(math.e)
    groups = unit // GROUP
    rows = [ref.shape[0] * unit for ref in kv_refs]
    starts = [sum(rows[:i]) for i in range(n_kv)]
    total = sum(rows)

    @pl.when(pl.program_id(0) == 0)
    def _():
        lanes = lane_index((GROUP, LANES))
        for ref, start in zip(kv_refs, starts):
            for index in range(ref.shape[0]):
                packed = ref[index, unit:, :].astype(jnp.float32)
                for group in range(groups):
                    tile, slot = group // (LANES // ROT), group % (LANES // ROT)
                    part = packed[:, tile * LANES : (tile + 1) * LANES]
                    low = pltpu.roll(part, (-slot * ROT) % LANES, 1) if slot else part
                    high = pltpu.roll(part, (PLAIN - slot * ROT) % LANES, 1)
                    both = jnp.where(lanes < ROT, low, jnp.where((lanes >= PLAIN) & (lanes < PLAIN + ROT), high, 0.0))
                    at_row = start + index * unit + group * GROUP
                    rot_ref[at_row : at_row + GROUP, :] = both.astype(jnp.bfloat16)

    weights = jnp.concatenate([key_w_ref[...], value_w_ref[...]], axis=1)
    for ref, start, count in zip(kv_refs, starts, rows):
        codes = ref[:, :unit, :].reshape(count, ref.shape[2])
        both = dot(codes, weights).astype(jnp.bfloat16)
        key_ref[start : start + count, :] = both[:, :LANES]
        val_ref[start : start + count, :] = both[:, LANES:]
    lanes = lane_index((total, LANES))
    queries = q_ref.shape[1]
    out_lanes = lane_index((queries, LANES))
    halves = []
    for head in range(2):
        own = (lanes < PLAIN) if head == 0 else (lanes >= PLAIN)
        k_full = jnp.where(own, key_ref[...], rot_ref[...])
        ones = (lanes == (PLAIN if head == 0 else 0)).astype(jnp.bfloat16)
        v_full = jnp.where(own, val_ref[...], ones)
        sum_lane = PLAIN if head == 0 else 0
        scores = dot_t(q_ref[head], k_full)
        if valid < unit:
            spot = lax.broadcasted_iota(jnp.int32, scores.shape, 1) % unit
            scores = jnp.where(spot < valid, scores, NEG)
        top = jnp.max(scores, axis=1, keepdims=True)
        if not first:
            before = state_ref[head]
            old_top = before[:, sum_lane + 1 : sum_lane + 2]
            top = jnp.maximum(top, old_top)
        probs = jnp.exp2((scores - top) * factor).astype(jnp.bfloat16)
        out = dot(probs, v_full)
        if not first:
            out = out + before * jnp.exp2((old_top - top) * factor)
        if last:
            halves.append(out * (1.0 / out[:, sum_lane : sum_lane + 1]))
        else:
            new_ref[head] = jnp.where(out_lanes == sum_lane + 1, top, out)
    if last:
        attended = jnp.where(out_lanes < PLAIN, halves[0], halves[1])
        gate = gate_ref[...].astype(jnp.float32)
        gated = (attended * (gate * (1.0 / (1.0 + jnp.exp(-gate))))).astype(jnp.bfloat16)
        keep_ref[...] = gated[: queries // 2]
        send_ref[...] = gated[queries // 2 :]


def attend(q_full, kv, key_w, value_w, state, gate, unit, valid):
    heads, queries, _ = q_full.shape
    first, last = state is None, gate is not None
    total = sum(part.shape[0] for part in kv) * unit
    whole = lambda part: pl.BlockSpec(part.shape, lambda g: (0,) * part.ndim)
    column = lambda count: pl.BlockSpec((count, LANES), lambda g: (0, g))
    heads_spec = pl.BlockSpec((2, queries, LANES), lambda g: (g, 0, 0))
    in_specs = [heads_spec] + [whole(part) for part in kv] + [column(key_w.shape[0])] * 2
    args = [q_full, *kv, key_w, value_w]
    if not first:
        in_specs.append(heads_spec)
        args.append(state)
    if last:
        in_specs.append(column(queries))
        args.append(gate)
        out_specs = [column(queries // 2)] * 2
        out_shape = [jax.ShapeDtypeStruct((queries // 2, heads * VALUE), jnp.bfloat16)] * 2
    else:
        out_specs = heads_spec
        out_shape = jax.ShapeDtypeStruct((heads, queries, LANES), jnp.float32)
    return pl.pallas_call(
        lambda *refs: attend_kernel(len(kv), unit, valid, first, last, *refs),
        grid=(heads // 2,),
        in_specs=in_specs,
        out_specs=out_specs,
        out_shape=out_shape,
        scratch_shapes=[pltpu.VMEM((total, LANES), jnp.bfloat16)] * 3,
        compiler_params=PARAMS,
        cost_estimate=cost(4 * heads * queries * total * LANES, 2**20),
        name="attend",
    )(*args)


def branch_kernel(mine_ref, theirs_ref, w_mine_ref, w_theirs_ref, far_ref, near_ref):
    near = near_ref.shape[0]
    far_ref[...] = (
        dot(mine_ref[near:, :], w_mine_ref[...]) + dot(theirs_ref[near:, :], w_theirs_ref[...])
    ).astype(jnp.bfloat16)
    near_ref[...] = dot(mine_ref[:near, :], w_mine_ref[...]) + dot(theirs_ref[:near, :], w_theirs_ref[...])


def norm_kernel(xors, me_ref, mod_ref, lat_ref, near_ref, far_ref, gain_ref, bias_ref, out_ref, vec_ref):
    fill_mod(me_ref, mod_ref, vec_ref, xors)
    branch = near_ref[...] + far_ref[...].astype(jnp.float32)
    blended = RESIDUAL * lat_ref[...].astype(jnp.float32) + vec_ref[4:5, :] * branch
    centred = blended - jnp.mean(blended, axis=-1, keepdims=True)
    variance = jnp.mean(centred * centred, axis=-1, keepdims=True)
    out_ref[...] = (centred * lax.rsqrt(variance + FLOOR) * gain_ref[...] + bias_ref[...]).astype(jnp.bfloat16)


def call(kernel, out_shape, args, scratch=(), flops=0, moved=0, smem=0, name=None):
    return pl.pallas_call(
        kernel,
        in_specs=[SMEM] * smem + [VMEM] * (len(args) - smem),
        out_specs=jax.tree.map(lambda _: VMEM, out_shape),
        out_shape=out_shape,
        scratch_shapes=list(scratch),
        compiler_params=PARAMS,
        cost_estimate=cost(flops, moved),
        name=name,
    )(*args)


def angle_tables(positions, rotated):
    lane = jnp.arange(LANES, dtype=jnp.int32)
    inverse = ROPE_BASE ** (-(lane % 8).astype(jnp.float32) / 8)
    on_column = (lane // 16) % 2 == 1
    place = jnp.where(on_column[None, :], (positions % GRID_W)[:, None], (positions // GRID_W)[:, None])
    angles = place.astype(jnp.float32) * inverse[None, :]
    sign = jnp.where((lane // 8) % 2 == 0, -1.0, 1.0)[None, :]
    cosine = jnp.where(rotated[:, None], jnp.cos(angles), 1.0)
    sine = jnp.where(rotated[:, None], jnp.sin(angles) * sign, 0.0)
    return cosine, sine


def per_device(
    latents,
    context,
    cond_vec,
    ctx_vec,
    shift_w,
    scale_w,
    modgate_w,
    query_down_weight,
    latent_down_weight,
    rot_down,
    gate_w,
    query_norm_gain,
    latent_norm_gain,
    query_plain_weight,
    query_rotary_weight,
    key_expand_weight,
    value_expand_weight,
    out_w,
    norm_gain,
    norm_bias,
):
    n_tp = lax.axis_size("tp")
    n_sp = lax.axis_size("sp")
    total = n_tp * n_sp
    sp_index, tp_index = lax.axis_index("sp"), lax.axis_index("tp")
    block, width = latents.shape
    f32, bf16 = jnp.float32, jnp.bfloat16

    def swap(array, mask):
        return lax.ppermute(array, ("sp", "tp"), [(i, i ^ mask) for i in range(total)])

    sp_masks = []
    mask = n_sp // 2
    while mask:
        sp_masks.append(mask * n_tp)
        mask //= 2
    tp_masks = []
    mask = n_tp // 2
    while mask:
        tp_masks.append(mask)
        mask //= 2
    me = tp_index.astype(jnp.int32).reshape(1)

    xors, blocks = [0], [latents]
    for mask in tp_masks:
        blocks = blocks + [swap(item, mask) for item in blocks]
        xors = xors + [x ^ mask for x in xors]
    out_w_pair = swap(out_w, 1)

    slab = shift_w.shape[0]
    cond = jnp.stack([cond_vec, ctx_vec])
    cond = lax.dynamic_slice_in_dim(cond, sp_index * slab, slab, 1)
    cond = jnp.concatenate([cond, jnp.zeros((6, slab), f32)], axis=0)
    columns = shift_w.shape[1]
    mod = call(mod_kernel, jax.ShapeDtypeStruct((8, columns), f32), (cond, shift_w, scale_w, modgate_w), name="mod")
    for mask in sp_masks:
        mod = mod + swap(mod, mask)
    mod = mod[None]
    for mask in tp_masks:
        mod = jnp.concatenate([mod, swap(mod, mask)], axis=0)
    vec_scratch = pltpu.VMEM((8, width), f32)

    ctx_rows = context.shape[0] // n_tp
    ctx_here = lax.dynamic_slice_in_dim(context, tp_index * ctx_rows, ctx_rows, 0)
    valid = block + ctx_rows
    unit = round_up(valid, GROUP)
    latent = latent_down_weight.shape[1]
    codes_w = jnp.concatenate([latent_down_weight, rot_down, jnp.zeros((width, LANES - ROT), bf16)], axis=1)
    row = jnp.arange(unit, dtype=jnp.int32)
    unit_cos, unit_sin = angle_tables((sp_index * n_tp + tp_index) * block + row, row < block)
    own = call(
        lambda *refs: codes_kernel(xors, *refs),
        jax.ShapeDtypeStruct((unit + GROUP, latent), bf16),
        (me, mod, latents, ctx_here, codes_w, latent_norm_gain.reshape(1, -1), unit_cos, unit_sin),
        scratch=(vec_scratch, pltpu.VMEM((unit, width), f32)),
        smem=1,
        name="codes",
    )

    near = own[None]
    for mask in sp_masks[:-1] + tp_masks[:-2]:
        near = jnp.concatenate([near, swap(near, mask)], axis=0)
    side_a, side_b = sp_masks[-1], tp_masks[-2]
    half = near.shape[0] // 2
    near_c = swap(near, 1)
    over_a = swap(near, side_a)
    over_b = swap(near, side_b)
    over_a_c = swap(over_a, 1)
    over_b_c = swap(over_b, 1)
    far_a = swap(over_b[:half], side_a)
    far_b = swap(over_a[half:], side_b)
    far_a_c = swap(far_a, 1)
    far_b_c = swap(far_b, 1)

    heads = gate_w.shape[1] // VALUE
    seq = block * n_tp
    order = jnp.concatenate([(tp_index ^ x) * block + jnp.arange(block, dtype=jnp.int32) for x in xors])
    q_cos, q_sin = angle_tables(sp_index * seq + order, jnp.ones((seq,), bool))
    rows_scratch = pltpu.VMEM((seq, width), f32)
    q_full = call(
        lambda *refs: query_kernel(xors, *refs),
        jax.ShapeDtypeStruct((heads, seq, LANES), bf16),
        (me, mod, *blocks, query_down_weight, query_norm_gain.reshape(1, -1), query_plain_weight, query_rotary_weight, q_cos, q_sin),
        scratch=(vec_scratch, rows_scratch),
        smem=1,
        flops=2 * seq * width * query_down_weight.shape[1],
        name="queries",
    )
    gate = call(
        lambda *refs: gate_kernel(xors, *refs),
        jax.ShapeDtypeStruct((seq, gate_w.shape[1]), bf16),
        (me, mod, *blocks, gate_w),
        scratch=(vec_scratch, rows_scratch),
        smem=1,
        flops=2 * seq * width * gate_w.shape[1],
        name="gate",
    )

    step = lambda kv, state, last: attend(
        q_full, kv, key_expand_weight, value_expand_weight, state, gate if last else None, unit, valid
    )
    state = step([near, near_c], None, False)
    state = step([over_a, over_b, over_a_c, over_b_c], state, False)
    keep, send = step([far_a, far_b, far_a_c, far_b_c], state, True)

    theirs = swap(send, 1)
    rows = keep.shape[0] // 2
    far, close = call(
        branch_kernel,
        [jax.ShapeDtypeStruct((rows, width), bf16), jax.ShapeDtypeStruct((keep.shape[0] - rows, width), f32)],
        (keep, theirs, out_w, out_w_pair),
        flops=4 * keep.shape[0] * keep.shape[1] * width,
        name="branch",
    )
    far = swap(far, tp_masks[-2])
    for mask in tp_masks[:-2][::-1]:
        close = close + far.astype(f32)
        rows = close.shape[0] // 2
        far = swap(close[rows:].astype(bf16), mask)
        close = close[:rows]
    return call(
        lambda *refs: norm_kernel(xors, *refs),
        jax.ShapeDtypeStruct((block, width), bf16),
        (me, mod, latents, close, far, norm_gain.reshape(1, -1), norm_bias.reshape(1, -1)),
        scratch=(vec_scratch,),
        smem=1,
        name="norm",
    )


def solution(mesh):
    in_specs = (
        P(("sp", "tp"), None),
        P("sp", None),
        P(),
        P(),
        P("sp", "tp"),
        P("sp", "tp"),
        P("sp", "tp"),
        P(),
        P(),
        P(),
        P(None, "tp"),
        P(),
        P(),
        P(None, "tp"),
        P(None, "tp"),
        P(None, "tp"),
        P(None, "tp"),
        P("tp", None),
        P(),
        P(),
    )
    return jax.shard_map(
        per_device, mesh=mesh, in_specs=in_specs, out_specs=P(("sp", "tp"), None), check_vma=False
    )
```
